32 devices in a mesh: ep: 8 (over z, x), tp: 4 (over y, core).
Axes of the slice: x: 2, y: 2, z: 4, core: 2. Of those that a mesh axis runs over, the one named last changes fastest.
Arguments:
- tokens: bfloat16 [256, 2048], P('ep'), may hold values from -6 to 6
- state: float32 [256, 16, 128, 128], P('ep', 'tp'), may hold values from -6 to 6
- norm_gain: float32 [2048], replicated, may hold values from 0.1 to 1.9
- w_query: bfloat16 [2048, 2048], P(None, 'tp'), may hold values from -0.125 to 0.125
- w_forget: bfloat16 [2048, 2048], P(None, 'tp'), may hold values from -0.125 to 0.125
- w_input: bfloat16 [2048, 2048], P(None, 'tp'), may hold values from -0.125 to 0.125
- w_outgate: bfloat16 [2048, 2048], P(None, 'tp'), may hold values from -0.125 to 0.125
- forget_floor: float32 [2048], P('tp'), may hold values from 0.05 to 0.95
- head_gain: float32 [128], replicated, may hold values from 0.1 to 1.9
- w_out: bfloat16 [2048, 2048], P('tp'), may hold values from -0.125 to 0.125
- ffn_gain: float32 [2048], replicated, may hold values from 0.1 to 1.9
- routes: int32 [256, 2], P('ep'), may hold values from 0 to 7, all different within a row; in each aligned block of 32 rows (0 to 31, 32 to 63, ...) at most 16 rows name the same one
- route_weights: float32 [256, 2], P('ep'), may hold values from 0.2 to 1
- expert_gate: bfloat16 [8, 2048, 5632], P('ep', None, 'tp'), may hold values from -0.125 to 0.125
- expert_up: bfloat16 [8, 2048, 5632], P('ep', None, 'tp'), may hold values from -0.125 to 0.125
- expert_down: bfloat16 [8, 5632, 2048], P('ep', 'tp'), may hold values from -0.078125 to 0.078125
- dense_gate: bfloat16 [2048, 5632], P(None, 'ep'), may hold values from -0.125 to 0.125
- dense_up: bfloat16 [2048, 5632], P(None, 'ep'), may hold values from -0.125 to 0.125
- dense_down: bfloat16 [5632, 2048], P('ep'), may hold values from -0.078125 to 0.078125
- dense_mix: float32 [2048], replicated, may hold values from -6 to 6
Outputs:
- mixed: bfloat16 [256, 2048], P('ep')
- new_state: float32 [256, 16, 128, 128], P('ep', 'tp')
The draws below stay inside these ranges and needn't reach their ends.
Inputs may be any that keep to these rules, and one draw needn't show every extreme that they name: `routes`: each row names 2 different experts; the rows of one index of ep name no expert more than 16 times, a bound that some block reaches.
All inputs are finite; a program needn't handle non-finite values.
Results may differ from the reference program's by a relative error of at most 0.014.
Values may be sent and summed in bfloat16 or wider, within the bound.
A program may use at most 128 MiB of HBM per device.

```python
import math
import jax
import jax.numpy as jnp
import numpy as np
from jax import lax

D = 2048
HEADS = 16
DK = 128
DV = 128
EFF = 5632
DFF = 5632
TOP = 2
SEQ_DEV = 32
EXPERTS = 8
CAP = 16
TOKENS = 256
N_EP = 8
N_TP = 4


def levels(own_key, extent, pieces, least, top_value):
    def one(axis_at, blocks):
        steps = jax.random.uniform(jax.random.fold_in(jax.random.fold_in(own_key, 6), axis_at), (blocks,), jnp.float32, least / len(pieces), top_value / len(pieces))
        return jnp.repeat(jnp.exp(steps), extent[axis_at] // blocks).reshape((-1,) + (1,) * (len(extent) - axis_at - 1))

    factor_of = one(*pieces[0])
    for cut in pieces[1:]:
        factor_of = factor_of * one(*cut)
    return factor_of


def routed_block(key, own, number, rows, amount, top, limit, lean):
    order = jax.random.permutation(key, amount)
    packed, usual = load_shares(amount, rows * top, limit, lean, True), load_shares(amount, rows * top, limit, lean, False)
    places = jnp.arange(amount)

    def named(sizes, offset_by):
        used = int((sizes > 0).sum())
        fixed = max(1, used // 4)
        moved = fixed + (places - fixed + offset_by * (used - fixed)) % max(1, amount - fixed)
        return jnp.zeros((amount,), jnp.int32).at[order[jnp.where(places < fixed, places, moved)]].set(jnp.asarray(sizes, jnp.int32))

    sizes = jnp.where(number % 4 == 0, named(packed, number // 4), named(usual, number - number // 4 - 1))
    mixed = jax.random.permutation(jax.random.fold_in(own, 3), amount)
    donor, receiver = mixed[0:amount // 2 * 2:2], mixed[1:amount // 2 * 2:2]
    slack = jnp.minimum(sizes[donor] - 1, limit - sizes[receiver]) // 2
    slack = jnp.where((donor == order[0]) | (receiver == order[0]) | (sizes[receiver] == 0), 0, jnp.maximum(slack, 0))
    moved = jax.random.randint(jax.random.fold_in(own, 4), (amount // 2,), 0, 1 << 20) % (slack + 1)
    sizes = sizes.at[donor].add(-moved).at[receiver].add(moved)
    items = jnp.searchsorted(jnp.cumsum(sizes), jnp.arange(rows * top), side="right").astype(jnp.int32)
    listing = items.reshape(top, rows).T
    listing = listing[jax.random.permutation(jax.random.fold_in(own, 1), rows)]
    offset_by = jax.random.randint(jax.random.fold_in(own, 2), (rows, 1), 0, top)
    return jnp.take_along_axis(listing, (jnp.arange(top)[None, :] + offset_by) % top, axis=1)


def load_shares(amount, total, reach, slope, full):
    weights = [(1 << 20) // math.isqrt(rank ** slope) + 1 for rank in range(1, amount + 1)]
    largest = reach if full else min(reach, max(-(-total // amount), total * weights[0] // sum(weights)))
    least = 1 if total - largest >= amount - 1 else 0
    holding, spare = [largest] + [least] * (amount - 1), total - largest - least * (amount - 1)
    while spare > 0:
        movable = [i for i in range(1, amount) if holding[i] < largest] or [i for i in range(1, amount) if holding[i] < reach]
        whole, budget = sum([weights[i] for i in movable]), spare
        for i in movable:
            extra = min(reach - holding[i], max(1, budget * weights[i] // whole), spare)
            holding[i] = holding[i] + extra
            spare = spare - extra
    return np.array(holding)


def gaussian(rng, shape, width, reach, shards=(), kind=jnp.bfloat16):
    array = width * jax.random.normal(rng, shape, jnp.float32)
    if shards:
        array = array * levels(rng, shape, shards, -0.22, 0.18)
    return jnp.clip(array, -reach, reach).astype(kind)


def setup_inputs(seed: int = 0) -> dict:
    key_list = jax.random.split(jax.random.key(seed), 21)
    tokens = gaussian(key_list[0], (TOKENS, D), 1.0, 6.0, ((0, 8),))
    state = gaussian(key_list[1], (TOKENS, HEADS, DK, DV), 1.0, 6.0, ((0, 8), (1, 4)), jnp.float32)
    norm_gain = jnp.clip(1.0 + 0.18 * jax.random.normal(key_list[2], (D,), jnp.float32), 0.1, 1.9)
    w_query = gaussian(key_list[3], (D, HEADS * DK), D ** -0.5, 0.125, ((1, 4),))
    w_forget = gaussian(key_list[4], (D, HEADS * DK), D ** -0.5, 0.125, ((1, 4),))
    w_input = gaussian(key_list[5], (D, HEADS * DV), D ** -0.5, 0.125, ((1, 4),))
    w_outgate = gaussian(key_list[6], (D, HEADS * DV), D ** -0.5, 0.125, ((1, 4),))
    forget_floor = jnp.clip(0.05 + 0.9 * jax.random.uniform(key_list[7], (HEADS * DK,), jnp.float32) ** levels(key_list[7], (HEADS * DK,), ((0, 4),), -0.2, 0.2), 0.05, 0.95)
    head_gain = jnp.clip(1.0 + 0.18 * jax.random.normal(key_list[8], (DV,), jnp.float32), 0.1, 1.9)
    w_out = gaussian(key_list[9], (HEADS * DV, D), (HEADS * DV) ** -0.5, 0.125, ((0, 4),))
    ffn_gain = jnp.clip(1.0 + 0.18 * jax.random.normal(key_list[10], (D,), jnp.float32), 0.1, 1.9)
    routes_keys = jax.random.split(jax.random.fold_in(key_list[11], 1), TOKENS // SEQ_DEV)
    routes_turns = jax.random.permutation(jax.random.fold_in(key_list[11], 3), TOKENS // SEQ_DEV)
    routes = jax.vmap(lambda own, number: routed_block(jax.random.fold_in(key_list[11], 2), own, number, SEQ_DEV, EXPERTS, TOP, CAP, 2))(routes_keys, routes_turns).reshape((TOKENS, TOP))
    route_weights = jnp.clip(0.2 + 0.8 * jax.random.uniform(key_list[12], (TOKENS, TOP), jnp.float32) ** levels(key_list[12], (TOKENS, TOP), ((0, 8),), -0.2, 0.2), 0.2, 1.0)
    expert_gate = gaussian(key_list[13], (EXPERTS, D, EFF), D ** -0.5, 0.125, ((0, 8), (2, 4)))
    expert_up = gaussian(key_list[14], (EXPERTS, D, EFF), D ** -0.5, 0.125, ((0, 8), (2, 4)))
    expert_down = gaussian(key_list[15], (EXPERTS, EFF, D), EFF ** -0.5, 0.078125, ((0, 8), (1, 4)))
    dense_gate = gaussian(key_list[16], (D, DFF), D ** -0.5, 0.125, ((1, 8),))
    dense_up = gaussian(key_list[17], (D, DFF), D ** -0.5, 0.125, ((1, 8),))
    dense_down = gaussian(key_list[18], (DFF, D), DFF ** -0.5, 0.078125, ((0, 8),))
    dense_mix = gaussian(key_list[19], (D,), 1.5, 6.0, (), jnp.float32)
    return dict(tokens=tokens, state=state, norm_gain=norm_gain, w_query=w_query, w_forget=w_forget, w_input=w_input, w_outgate=w_outgate, forget_floor=forget_floor, head_gain=head_gain, w_out=w_out, ffn_gain=ffn_gain, routes=routes, route_weights=route_weights, expert_gate=expert_gate, expert_up=expert_up, expert_down=expert_down, dense_gate=dense_gate, dense_up=dense_up, dense_down=dense_down, dense_mix=dense_mix)


EPS = 1e-06

def rounded(value):
    return lax.optimization_barrier(value.astype(jnp.bfloat16)).astype(jnp.float32)

def rms_norm(value, gain):
    return value * lax.rsqrt(lax.optimization_barrier(jnp.mean(value * value, axis=-1, keepdims=True)) + EPS) * gain

def make_table(group_routes, experts, capacity):
    flat = group_routes.reshape(-1)
    onehot = (flat[:, None] == jnp.arange(experts, dtype=jnp.int32)[None, :]).astype(jnp.int32)
    before = jnp.cumsum(onehot, axis=0) - onehot
    slot = lax.optimization_barrier(jnp.sum(before * onehot, axis=1))
    where = flat * capacity + slot
    return (where[:, None] == jnp.arange(experts * capacity, dtype=jnp.int32)[None, :]).astype(jnp.float32)

def reference(tokens, state, norm_gain, w_query, w_forget, w_input, w_outgate, forget_floor, head_gain, w_out, ffn_gain, routes, route_weights, expert_gate, expert_up, expert_down, dense_gate, dense_up, dense_down, dense_mix):
    resid_in = tokens.astype(jnp.float32)
    normed = rms_norm(resid_in, norm_gain).astype(jnp.bfloat16)
    zq = jnp.dot(normed, w_query, preferred_element_type=jnp.float32)
    zf = jnp.dot(normed, w_forget, preferred_element_type=jnp.float32)
    zi = jnp.dot(normed, w_input, preferred_element_type=jnp.float32)
    zg = jnp.dot(normed, w_outgate, preferred_element_type=jnp.float32)
    logf = jnp.logaddexp(jax.nn.log_sigmoid(zf), jnp.log(forget_floor) + jax.nn.log_sigmoid(-zf))
    logf = logf.reshape(TOKENS, HEADS, DK)
    query = jax.nn.silu(zq).reshape(TOKENS, HEADS, DK)
    keep = jnp.exp(logf)
    write = -jnp.expm1(logf)
    values = zi.reshape(TOKENS, HEADS, DV)
    new_state = keep[..., None] * state + write[..., None] * values[:, :, None, :]
    read = jnp.einsum('thk,thkv->thv', query, new_state, precision=lax.Precision.HIGHEST)
    read = rms_norm(read, head_gain).reshape(TOKENS, HEADS * DV)
    headout = (read * jax.nn.silu(zg)).astype(jnp.bfloat16)
    blocks = jnp.einsum('tnc,ncd->ntd', headout.reshape(TOKENS, N_TP, -1).astype(jnp.float32), w_out.reshape(N_TP, -1, D).astype(jnp.float32))
    mixout = lax.optimization_barrier(jnp.sum(rounded(blocks), axis=0))
    resid = resid_in + mixout
    ffn_in = rms_norm(resid, ffn_gain).astype(jnp.bfloat16)
    group_routes = routes.reshape(N_EP, SEQ_DEV, TOP)
    tables = jax.vmap(lambda r: make_table(r, EXPERTS, CAP))(group_routes)
    repeated = jnp.repeat(ffn_in.reshape(N_EP, SEQ_DEV, D), TOP, axis=1).astype(jnp.float32)
    sent = jnp.einsum('grp,grd->gpd', tables, repeated).astype(jnp.bfloat16)
    arrived = sent.reshape(N_EP, EXPERTS, CAP, D).transpose(1, 0, 2, 3).reshape(EXPERTS, N_EP * CAP, D)

    def one_expert(items):
        rows, gate_w, up_w, down_w = items
        gate = jnp.dot(rows, gate_w, preferred_element_type=jnp.float32)
        upper = jnp.dot(rows, up_w, preferred_element_type=jnp.float32)
        hidden = (jax.nn.silu(gate) * upper).astype(jnp.bfloat16)
        parts = jnp.einsum('rnc,ncd->nrd', hidden.reshape(rows.shape[0], N_TP, -1).astype(jnp.float32), down_w.reshape(N_TP, -1, D).astype(jnp.float32))
        return lax.optimization_barrier(jnp.sum(rounded(parts), axis=0)).astype(jnp.bfloat16)
    outputs = lax.map(one_expert, (arrived, expert_gate, expert_up, expert_down))
    back = outputs.reshape(EXPERTS, N_EP, CAP, D).transpose(1, 0, 2, 3).reshape(N_EP, EXPERTS * CAP, D)
    picked = jnp.einsum('grp,gpd->grd', tables, back.astype(jnp.float32))
    weighted = picked * route_weights.reshape(N_EP, SEQ_DEV * TOP)[:, :, None]
    moe = lax.optimization_barrier(jnp.sum(weighted.reshape(N_EP, SEQ_DEV, TOP, D), axis=2)).reshape(TOKENS, D)
    dgate = jnp.dot(ffn_in, dense_gate, preferred_element_type=jnp.float32)
    dupper = jnp.dot(ffn_in, dense_up, preferred_element_type=jnp.float32)
    dense_hidden = (jax.nn.silu(dgate) * dupper).astype(jnp.bfloat16)
    dense = rounded(jnp.dot(dense_hidden, dense_down, preferred_element_type=jnp.float32))
    mixed = (resid + moe + jax.nn.sigmoid(dense_mix) * dense).astype(jnp.bfloat16)
    return (mixed, new_state)
```

```python
import functools

import jax
import jax.numpy as jnp
from jax import lax
from jax.experimental import pallas as pl
from jax.experimental.pallas import tpu as pltpu
from jax.sharding import PartitionSpec as P

EPS = 1e-06


def rms_norm(value, gain):
    return value * lax.rsqrt(jnp.mean(value * value, axis=-1, keepdims=True) + EPS) * gain


def make_table(local_routes, experts, capacity):
    flat = local_routes.reshape(-1)
    onehot = (flat[:, None] == jnp.arange(experts, dtype=jnp.int32)[None, :]).astype(jnp.int32)
    before = jnp.cumsum(onehot, axis=0) - onehot
    slot = jnp.sum(before * onehot, axis=1)
    where = flat * capacity + slot
    return (where[:, None] == jnp.arange(experts * capacity, dtype=jnp.int32)[None, :]).astype(
        jnp.bfloat16
    )


def channel_kernel(
    ep_size,
    tp_size,
    tok_ref,
    bt_ref,
    gain_ref,
    mix_ref,
    routes_ref,
    rw_ref,
    eg_hbm,
    eu_hbm,
    ed_hbm,
    dg_hbm,
    du_hbm,
    dd_hbm,
    out_ref,
    eg,
    eu,
    ed,
    dg,
    du,
    dd,
    rs_buf,
    xg,
    wt,
    wg,
    wcol,
    x2d,
    hid,
    dhid,
    resid_ref,
    cbuf,
    crecv,
    ysend,
    yrecv,
    esend,
    erecv,
    fbuf,
    ld_sem,
    rs_s,
    rs_r,
    w_s,
    w_r,
    ag_s,
    g_r,
    gy_s,
    gc_s,
    cr_s,
    cr_r,
    yr_s,
    yr_r,
    er_s,
    er_r,
    f_s,
    f_r,
):
    E, T = ep_size, tp_size
    Y = T // 2
    e, t = lax.axis_index("ep"), lax.axis_index("tp")
    y, c = t // 2, t % 2
    partner = y * 2 + (1 - c)
    rows, width = resid_ref.shape
    seqs = T * rows
    units = dg.shape[0]
    hidden_units = eg.shape[1]

    def rcopy(src, dst, ssem, rsem, ee, tt):
        return pltpu.make_async_remote_copy(
            src_ref=src,
            dst_ref=dst,
            send_sem=ssem,
            recv_sem=rsem,
            device_id={"ep": ee, "tp": tt},
            device_id_type=pl.DeviceIdType.MESH,
        )

    mine = pl.ds(pl.multiple_of(t * units, 16), units)
    loads = [
        pltpu.make_async_copy(dg_hbm.at[mine], dg, ld_sem.at[0]),
        pltpu.make_async_copy(du_hbm.at[mine], du, ld_sem.at[1]),
        pltpu.make_async_copy(eg_hbm, eg, ld_sem.at[2]),
        pltpu.make_async_copy(eu_hbm, eu, ld_sem.at[3]),
        pltpu.make_async_copy(ed_hbm, ed, ld_sem.at[4]),
        pltpu.make_async_copy(dd_hbm.at[mine], dd, ld_sem.at[5]),
    ]
    barrier = pltpu.get_barrier_semaphore()
    for i in range(1, E):
        pl.semaphore_signal(
            barrier, inc=1, device_id={"ep": (e + i) % E, "tp": t}, device_id_type=pl.DeviceIdType.MESH
        )
    for i in range(1, T):
        pl.semaphore_signal(
            barrier, inc=1, device_id={"ep": e, "tp": (t + i) % T}, device_id_type=pl.DeviceIdType.MESH
        )
    for cp in loads:
        cp.start()

    which = lax.broadcasted_iota(jnp.int32, (E, seqs), 0)
    table = jnp.zeros((E, seqs), jnp.float32)
    for k in range(routes_ref.shape[0]):
        table = table + jnp.where(routes_ref[k : k + 1, :] == which, rw_ref[k : k + 1, :], 0.0)
    wt[...] = jnp.zeros(wt.shape, jnp.float32)
    wt[:, :seqs] = table

    pl.semaphore_wait(barrier, E + T - 2)

    sends = []
    for i in range(1, T):
        j = (t + i) % T
        cp = rcopy(bt_ref.at[j], rs_buf.at[t], rs_s.at[j], rs_r.at[t], e, j)
        cp.start()
        sends.append(cp)
    far = [E // 2]
    for i in range(1, E // 2):
        far = [i, E - i] + far
    near, far = far, far[::-1]
    for i in far:
        j = (e + i) % E
        cp = rcopy(wt, wg.at[e], w_s.at[j], w_r.at[e], j, t)
        cp.start()
        sends.append(cp)

    resid = tok_ref[t].astype(jnp.float32) + bt_ref[t].astype(jnp.float32)
    for i in range(1, T):
        j = (t + i) % T
        rcopy(rs_buf.at[j], rs_buf.at[j], rs_s.at[j], rs_r.at[j], e, j).wait_recv()
        resid = resid + rs_buf[j].astype(jnp.float32)
    resid_ref[...] = resid
    normed = rms_norm(resid, gain_ref[...])
    xg[e, t] = normed.astype(jnp.bfloat16)

    for i in far:
        j = (e + i) % E
        cp = rcopy(xg.at[e, t], xg.at[e, t], ag_s.at[j], g_r.at[e, t], j, t)
        cp.start()
        sends.append(cp)

    def forward(source):
        for k in range(1, Y):
            yy = (y + k) % Y
            cp = rcopy(
                xg.at[source, t], xg.at[source, t], gy_s.at[source, yy], g_r.at[source, t], e, yy * 2 + c
            )
            cp.start()
            sends.append(cp)
        forward_core(source, y)

    def forward_core(source, yy):
        col = yy * 2 + c
        cp = rcopy(
            xg.at[source, col], xg.at[source, col], gc_s.at[source, yy], g_r.at[source, col], e, partner
        )
        cp.start()
        sends.append(cp)

    def arrived(source, col):
        rcopy(
            xg.at[source, col], xg.at[source, col], ag_s.at[source], g_r.at[source, col], source, col
        ).wait_recv()

    forward(e)
    order = [0] + near
    diag = lax.broadcasted_iota(jnp.int32, (seqs, wt.shape[1]), 0) == lax.broadcasted_iota(
        jnp.int32, (seqs, wt.shape[1]), 1
    )
    for i in near:
        source = (e + i) % E
        arrived(source, t)
        forward(source)
    for i in order:
        source = (e + i) % E
        for k in range(1, Y):
            yy = (y + k) % Y
            arrived(source, yy * 2 + c)
            forward_core(source, yy)
        if i == 0:
            line = wt[pl.ds(e, 1), :]
        else:
            rcopy(wg.at[source], wg.at[source], w_s.at[source], w_r.at[source], source, t).wait_recv()
            line = wg[source, pl.ds(e, 1), :]
        column = jnp.sum(jnp.where(diag, line, 0.0), axis=1, keepdims=True)
        at = pl.ds(pl.multiple_of(source * seqs, seqs), seqs)
        wcol[at, :] = jnp.broadcast_to(column, (seqs, wcol.shape[1]))
    for i in order:
        source = (e + i) % E
        for yy in range(Y):
            arrived(source, yy * 2 + (1 - c))
        at = pl.ds(pl.multiple_of(source * seqs, seqs), seqs)
        x2d[at, :] = xg[source].astype(jnp.float32).reshape(seqs, width).astype(jnp.bfloat16)

    across = (((1,), (1,)), ((), ()))
    loads[0].wait()
    loads[1].wait()
    dgate = lax.dot_general(x2d[...], dg[...], across, preferred_element_type=jnp.float32)
    dupper = lax.dot_general(x2d[...], du[...], across, preferred_element_type=jnp.float32)
    dhid[...] = (jax.nn.silu(dgate) * dupper).astype(jnp.bfloat16)
    loads[2].wait()
    loads[3].wait()

    def hidden_at(cols):
        gate = jnp.dot(x2d[...], eg[:, cols], preferred_element_type=jnp.float32)
        upper = jnp.dot(x2d[...], eu[:, cols], preferred_element_type=jnp.float32)
        hid[:, cols] = (jax.nn.silu(gate) * upper).astype(jnp.bfloat16)

    step = 256
    whole_steps = hidden_units // step

    @pl.loop(0, whole_steps)
    def _(n):
        hidden_at(pl.ds(pl.multiple_of(n * step, step), step))

    if hidden_units % step:
        hidden_at(pl.ds(whole_steps * step, hidden_units % step))
    loads[4].wait()
    loads[5].wait()

    @pl.loop(0, width // step)
    def _(n):
        cols = pl.ds(pl.multiple_of(n * step, step), step)
        expert = jnp.dot(hid[...], ed[:, cols], preferred_element_type=jnp.float32)
        dense = jnp.dot(dhid[...], dd[:, cols], preferred_element_type=jnp.float32)
        both = wcol[:, :1] * expert + jax.nn.sigmoid(mix_ref[:, cols]) * dense
        both = both.reshape(E, T, rows, step).astype(jnp.bfloat16)
        for j in range(T):
            cbuf[j % 2, j // 2, :, :, cols] = both[:, j]

    others = []
    for k in range(Y):
        yy = (y + 1 + k) % Y
        cp = rcopy(cbuf.at[1 - c, yy], crecv.at[yy], cr_s.at[yy], cr_r.at[yy], e, partner)
        cp.start()
        sends.append(cp)
        others.append(yy)

    def core_sum(yy, block):
        return cbuf[c, yy, block].astype(jnp.float32) + crecv[yy, block].astype(jnp.float32)

    def core_arrived(yy):
        rcopy(crecv.at[yy], crecv.at[yy], cr_s.at[yy], cr_r.at[yy], e, partner).wait_recv()

    for yy in others[:-1]:
        core_arrived(yy)
        for i in far + [0]:
            block = (e + i) % E
            ysend[yy, block] = core_sum(yy, block).astype(jnp.bfloat16)
            cp = rcopy(
                ysend.at[yy, block], yrecv.at[y, block], yr_s.at[yy, block], yr_r.at[y, block], e, yy * 2 + c
            )
            cp.start()
            sends.append(cp)
    core_arrived(y)
    total = None
    for i in far + [0]:
        block = (e + i) % E
        total = core_sum(y, block)
        for yy in others[:-1]:
            rcopy(
                yrecv.at[yy, block], yrecv.at[yy, block], yr_s.at[yy, block], yr_r.at[yy, block], e, yy * 2 + c
            ).wait_recv()
            total = total + yrecv[yy, block].astype(jnp.float32)
        if i:
            esend[block] = total.astype(jnp.bfloat16)
            cp = rcopy(esend.at[block], erecv.at[e], er_s.at[block], er_r.at[e], block, t)
            cp.start()
            sends.append(cp)
    total = total + resid_ref[...]
    for i in near:
        source = (e + i) % E
        rcopy(erecv.at[source], erecv.at[source], er_s.at[source], er_r.at[source], source, t).wait_recv()
        total = total + erecv[source].astype(jnp.float32)
    fbuf[t] = total.astype(jnp.bfloat16)
    for i in range(1, T):
        j = (t + i) % T
        cp = rcopy(fbuf.at[t], fbuf.at[t], f_s.at[j], f_r.at[t], e, j)
        cp.start()
        sends.append(cp)
    for i in range(1, T):
        j = (t + i) % T
        rcopy(fbuf.at[j], fbuf.at[j], f_s.at[j], f_r.at[j], e, j).wait_recv()
    out_ref[...] = fbuf[...]
    for cp in sends:
        cp.wait_send()


def channel_mixers(tokens, term, ffn_gain, dense_mix, routes, route_weights, expert, dense):
    E, T = lax.axis_size("ep"), lax.axis_size("tp")
    Y = T // 2
    seqs, width = tokens.shape
    rows = seqs // T
    eg, eu, ed = expert
    dg, du, dd = dense
    units = dg.shape[0] // T
    hidden_units = eg.shape[1]
    bf, f32 = jnp.bfloat16, jnp.float32
    vmem, dma = pltpu.VMEM, pltpu.SemaphoreType.DMA
    block = (rows, width)
    total = E * seqs
    vm = pl.BlockSpec(memory_space=pltpu.VMEM)
    hbm = pl.BlockSpec(memory_space=pl.ANY)
    out = pl.pallas_call(
        functools.partial(channel_kernel, E, T),
        out_shape=jax.ShapeDtypeStruct((T,) + block, bf),
        in_specs=[vm] * 6 + [hbm] * 6,
        out_specs=vm,
        scratch_shapes=[
            vmem(eg.shape, bf),
            vmem(eu.shape, bf),
            vmem(ed.shape, bf),
            vmem((units, width), bf),
            vmem((units, width), bf),
            vmem((units, width), bf),
            vmem((T,) + block, bf),
            vmem((E, T) + block, bf),
            vmem((E, 128), f32),
            vmem((E, E, 128), f32),
            vmem((total, 128), f32),
            vmem((total, width), bf),
            vmem((total, hidden_units), bf),
            vmem((total, units), bf),
            vmem(block, f32),
            vmem((2, Y, E) + block, bf),
            vmem((Y, E) + block, bf),
            vmem((Y, E) + block, bf),
            vmem((Y, E) + block, bf),
            vmem((E,) + block, bf),
            vmem((E,) + block, bf),
            vmem((T,) + block, bf),
            dma((6,)),
            dma((T,)),
            dma((T,)),
            dma((E,)),
            dma((E,)),
            dma((E,)),
            dma((E, T)),
            dma((E, Y)),
            dma((E, Y)),
            dma((Y,)),
            dma((Y,)),
            dma((Y, E)),
            dma((Y, E)),
            dma((E,)),
            dma((E,)),
            dma((T,)),
            dma((T,)),
        ],
        compiler_params=pltpu.CompilerParams(
            collective_id=0, has_side_effects=True, vmem_limit_bytes=50 * 1024 * 1024
        ),
        name="channel_mixers",
    )(
        tokens.reshape((T,) + block),
        term.reshape((T,) + block),
        ffn_gain.reshape(1, width),
        dense_mix.reshape(1, width),
        routes.T,
        route_weights.T,
        eg,
        eu,
        ed,
        dg,
        du,
        dd,
    )
    return out.reshape(seqs, width)


def local(
    tokens,
    state,
    norm_gain,
    w_query,
    w_forget,
    w_input,
    w_outgate,
    forget_floor,
    head_gain,
    w_out,
    ffn_gain,
    routes,
    route_weights,
    expert_gate,
    expert_up,
    expert_down,
    dense_gate,
    dense_up,
    dense_down,
    dense_mix,
):
    seqs, width = tokens.shape
    local_heads = state.shape[1]
    key_size = state.shape[2]
    value_size = state.shape[3]
    resid_in = tokens.astype(jnp.float32)
    normed = rms_norm(resid_in, norm_gain).astype(jnp.bfloat16)
    zq = jnp.dot(normed, w_query, preferred_element_type=jnp.float32)
    zf = jnp.dot(normed, w_forget, preferred_element_type=jnp.float32)
    zi = jnp.dot(normed, w_input, preferred_element_type=jnp.float32)
    zg = jnp.dot(normed, w_outgate, preferred_element_type=jnp.float32)
    logf = jnp.logaddexp(jax.nn.log_sigmoid(zf), jnp.log(forget_floor) + jax.nn.log_sigmoid(-zf))
    logf = logf.reshape(seqs, local_heads, key_size)
    query = jax.nn.silu(zq).reshape(seqs, local_heads, key_size)
    keep = jnp.exp(logf)
    write = -jnp.expm1(logf)
    values = zi.reshape(seqs, local_heads, value_size)
    new_state = keep[..., None] * state + write[..., None] * values[:, :, None, :]
    read = jnp.einsum("thk,thkv->thv", query, new_state, precision=lax.Precision.HIGHEST)
    read = rms_norm(read, head_gain).reshape(seqs, local_heads * value_size)
    headout = (read * jax.nn.silu(zg)).astype(jnp.bfloat16)
    block_term = jnp.dot(headout, w_out, preferred_element_type=jnp.float32)
    ways = lax.axis_size("tp")
    if ways % 2 == 0 and seqs % (8 * ways) == 0 and dense_gate.shape[1] % (16 * ways) == 0:
        mixed = channel_mixers(
            tokens,
            block_term.astype(jnp.bfloat16),
            ffn_gain,
            dense_mix,
            routes,
            route_weights,
            (expert_gate[0], expert_up[0], expert_down[0]),
            (dense_gate.T, dense_up.T, dense_down),
        )
        return (mixed, new_state)
    block_term = block_term.astype(jnp.bfloat16).astype(jnp.float32)
    mixout = lax.psum(block_term.astype(jnp.bfloat16), "tp").astype(jnp.float32)
    resid = resid_in + mixout
    ffn_in = rms_norm(resid, ffn_gain).astype(jnp.bfloat16)
    piece = lax.all_gather(ffn_in, "ep", axis=0, tiled=True)
    dgate = jnp.dot(piece, dense_gate, preferred_element_type=jnp.float32)
    dupper = jnp.dot(piece, dense_up, preferred_element_type=jnp.float32)
    dense_hidden = (jax.nn.silu(dgate) * dupper).astype(jnp.bfloat16)
    rows = dense_hidden
    summed = lax.psum_scatter(
        jnp.dot(rows, dense_down, preferred_element_type=jnp.float32).astype(jnp.bfloat16),
        "ep",
        scatter_dimension=0,
        tiled=True,
    )
    dense = summed.astype(jnp.float32)
    experts = lax.axis_size("ep") * expert_gate.shape[0]
    top = routes.shape[1]
    capacity = 2 * seqs * top // experts
    table = make_table(routes, experts, capacity)
    repeated = jnp.repeat(ffn_in, top, axis=0)
    sent = jnp.dot(table.T, repeated, preferred_element_type=jnp.float32).astype(jnp.bfloat16)
    sent = sent.reshape(experts, capacity, width)
    arrived = lax.all_to_all(sent, "ep", split_axis=0, concat_axis=0, tiled=True)
    sources, items, _ = arrived.shape
    rows = arrived.reshape(sources * items, width)
    gate = jnp.dot(rows, expert_gate[0], preferred_element_type=jnp.float32)
    upper = jnp.dot(rows, expert_up[0], preferred_element_type=jnp.float32)
    hidden = (jax.nn.silu(gate) * upper).astype(jnp.bfloat16)
    part = jnp.dot(hidden, expert_down[0], preferred_element_type=jnp.float32)
    part = part.astype(jnp.bfloat16).astype(jnp.float32)
    summed_parts = lax.psum(part.astype(jnp.bfloat16), "tp")
    results = summed_parts.reshape(sources, items, width)
    back = lax.all_to_all(results, "ep", split_axis=0, concat_axis=0, tiled=True)
    picked = jnp.dot(
        table, back.reshape(experts * capacity, width), preferred_element_type=jnp.float32
    )
    weighted = picked * route_weights.reshape(seqs * top)[:, None]
    moe = jnp.sum(weighted.reshape(seqs, top, width), axis=1)
    mixed = (resid + moe + jax.nn.sigmoid(dense_mix) * dense).astype(jnp.bfloat16)
    return (mixed, new_state)


def solution(mesh):
    in_specs = (
        P("ep", None),
        P("ep", "tp", None, None),
        P(),
        P(None, "tp"),
        P(None, "tp"),
        P(None, "tp"),
        P(None, "tp"),
        P("tp"),
        P(),
        P("tp", None),
        P(),
        P("ep", None),
        P("ep", None),
        P("ep", None, "tp"),
        P("ep", None, "tp"),
        P("ep", "tp", None),
        P(None, "ep"),
        P(None, "ep"),
        P("ep", None),
        P(),
    )
    out_specs = (P("ep", None), P("ep", "tp", None, None))
    return jax.shard_map(local, mesh=mesh, in_specs=in_specs, out_specs=out_specs, check_vma=False)
```

```python
import functools

import jax
import jax.numpy as jnp
from jax import lax
from jax.experimental import pallas as pl
from jax.experimental.pallas import tpu as pltpu
from jax.sharding import PartitionSpec as P

EPS = 1e-06


def rms_norm(value, gain):
    return value * lax.rsqrt(jnp.mean(value * value, axis=-1, keepdims=True) + EPS) * gain


def make_table(local_routes, experts, capacity):
    flat = local_routes.reshape(-1)
    onehot = (flat[:, None] == jnp.arange(experts, dtype=jnp.int32)[None, :]).astype(jnp.int32)
    before = jnp.cumsum(onehot, axis=0) - onehot
    slot = jnp.sum(before * onehot, axis=1)
    where = flat * capacity + slot
    return (where[:, None] == jnp.arange(experts * capacity, dtype=jnp.int32)[None, :]).astype(
        jnp.bfloat16
    )


def channel_kernel(
    ep_size,
    tp_size,
    tok_ref,
    bt_ref,
    gain_ref,
    mix_ref,
    routes_ref,
    rw_ref,
    eg_hbm,
    eu_hbm,
    ed_hbm,
    dg_hbm,
    du_hbm,
    dd_hbm,
    out_ref,
    eg,
    eu,
    ed,
    dg,
    du,
    dd,
    rs_buf,
    xg,
    wt,
    wg,
    wcol,
    x2d,
    hid,
    dhid,
    resid_ref,
    cbuf,
    crecv,
    ysend,
    yrecv,
    esend,
    erecv,
    fbuf,
    ld_sem,
    rs_s,
    rs_r,
    w_s,
    w_r,
    ag_s,
    g_r,
    gy_s,
    gc_s,
    cr_s,
    cr_r,
    yr_s,
    yr_r,
    er_s,
    er_r,
    f_s,
    f_r,
):
    E, T = ep_size, tp_size
    Y = T // 2
    e, t = lax.axis_index("ep"), lax.axis_index("tp")
    y, c = t // 2, t % 2
    partner = y * 2 + (1 - c)
    rows, width = resid_ref.shape
    seqs = T * rows
    units = dg.shape[0]
    hidden_units = eg.shape[1]

    def rcopy(src, dst, ssem, rsem, ee, tt):
        return pltpu.make_async_remote_copy(
            src_ref=src,
            dst_ref=dst,
            send_sem=ssem,
            recv_sem=rsem,
            device_id={"ep": ee, "tp": tt},
            device_id_type=pl.DeviceIdType.MESH,
        )

    mine = pl.ds(pl.multiple_of(t * units, 16), units)
    loads = [
        pltpu.make_async_copy(dg_hbm.at[mine], dg, ld_sem.at[0]),
        pltpu.make_async_copy(du_hbm.at[mine], du, ld_sem.at[1]),
        pltpu.make_async_copy(eg_hbm, eg, ld_sem.at[2]),
        pltpu.make_async_copy(eu_hbm, eu, ld_sem.at[3]),
        pltpu.make_async_copy(ed_hbm, ed, ld_sem.at[4]),
        pltpu.make_async_copy(dd_hbm.at[mine], dd, ld_sem.at[5]),
    ]
    barrier = pltpu.get_barrier_semaphore()
    for i in range(1, E):
        pl.semaphore_signal(
            barrier, inc=1, device_id={"ep": (e + i) % E, "tp": t}, device_id_type=pl.DeviceIdType.MESH
        )
    for i in range(1, T):
        pl.semaphore_signal(
            barrier, inc=1, device_id={"ep": e, "tp": (t + i) % T}, device_id_type=pl.DeviceIdType.MESH
        )
    for cp in loads:
        cp.start()

    which = lax.broadcasted_iota(jnp.int32, (E, seqs), 0)
    table = jnp.zeros((E, seqs), jnp.float32)
    for k in range(routes_ref.shape[0]):
        table = table + jnp.where(routes_ref[k : k + 1, :] == which, rw_ref[k : k + 1, :], 0.0)
    wt[...] = jnp.zeros(wt.shape, jnp.float32)
    wt[:, :seqs] = table

    pl.semaphore_wait(barrier, E + T - 2)

    sends = []
    for i in range(1, T):
        j = (t + i) % T
        cp = rcopy(bt_ref.at[j], rs_buf.at[t], rs_s.at[j], rs_r.at[t], e, j)
        cp.start()
        sends.append(cp)
    far = [E // 2]
    for i in range(1, E // 2):
        far = [i, E - i] + far
    near, far = far, far[::-1]
    for i in far:
        j = (e + i) % E
        cp = rcopy(wt, wg.at[e], w_s.at[j], w_r.at[e], j, t)
        cp.start()
        sends.append(cp)

    resid = tok_ref[t].astype(jnp.float32) + bt_ref[t].astype(jnp.float32)
    for i in range(1, T):
        j = (t + i) % T
        rcopy(rs_buf.at[j], rs_buf.at[j], rs_s.at[j], rs_r.at[j], e, j).wait_recv()
        resid = resid + rs_buf[j].astype(jnp.float32)
    resid_ref[...] = resid
    normed = rms_norm(resid, gain_ref[...])
    xg[e, t] = normed.astype(jnp.bfloat16)

    for i in far:
        j = (e + i) % E
        cp = rcopy(xg.at[e, t], xg.at[e, t], ag_s.at[j], g_r.at[e, t], j, t)
        cp.start()
        sends.append(cp)

    def forward(source):
        for k in range(1, Y):
            yy = (y + k) % Y
            cp = rcopy(
                xg.at[source, t], xg.at[source, t], gy_s.at[source, yy], g_r.at[source, t], e, yy * 2 + c
            )
            cp.start()
            sends.append(cp)
        forward_core(source, y)

    def forward_core(source, yy):
        col = yy * 2 + c
        cp = rcopy(
            xg.at[source, col], xg.at[source, col], gc_s.at[source, yy], g_r.at[source, col], e, partner
        )
        cp.start()
        sends.append(cp)

    def arrived(source, col):
        rcopy(
            xg.at[source, col], xg.at[source, col], ag_s.at[source], g_r.at[source, col], source, col
        ).wait_recv()

    forward(e)
    order = [0] + near
    diag = lax.broadcasted_iota(jnp.int32, (seqs, wt.shape[1]), 0) == lax.broadcasted_iota(
        jnp.int32, (seqs, wt.shape[1]), 1
    )
    for i in near:
        source = (e + i) % E
        arrived(source, t)
        forward(source)
    for i in order:
        source = (e + i) % E
        for k in range(1, Y):
            yy = (y + k) % Y
            arrived(source, yy * 2 + c)
            forward_core(source, yy)
        if i == 0:
            line = wt[pl.ds(e, 1), :]
        else:
            rcopy(wg.at[source], wg.at[source], w_s.at[source], w_r.at[source], source, t).wait_recv()
            line = wg[source, pl.ds(e, 1), :]
        column = jnp.sum(jnp.where(diag, line, 0.0), axis=1, keepdims=True)
        at = pl.ds(pl.multiple_of(source * seqs, seqs), seqs)
        wcol[at, :] = jnp.broadcast_to(column, (seqs, wcol.shape[1]))
    for i in order:
        source = (e + i) % E
        for yy in range(Y):
            arrived(source, yy * 2 + (1 - c))
        at = pl.ds(pl.multiple_of(source * seqs, seqs), seqs)
        x2d[at, :] = xg[source].astype(jnp.float32).reshape(seqs, width).astype(jnp.bfloat16)

    across = (((1,), (1,)), ((), ()))
    loads[0].wait()
    loads[1].wait()
    dgate = lax.dot_general(x2d[...], dg[...], across, preferred_element_type=jnp.float32)
    dupper = lax.dot_general(x2d[...], du[...], across, preferred_element_type=jnp.float32)
    dhid[...] = (jax.nn.silu(dgate) * dupper).astype(jnp.bfloat16)
    loads[2].wait()
    loads[3].wait()

    def hidden_at(cols):
        gate = jnp.dot(x2d[...], eg[:, cols], preferred_element_type=jnp.float32)
        upper = jnp.dot(x2d[...], eu[:, cols], preferred_element_type=jnp.float32)
        hid[:, cols] = (jax.nn.silu(gate) * upper).astype(jnp.bfloat16)

    step = 256
    whole_steps = hidden_units // step

    @pl.loop(0, whole_steps)
    def _(n):
        hidden_at(pl.ds(pl.multiple_of(n * step, step), step))

    if hidden_units % step:
        hidden_at(pl.ds(whole_steps * step, hidden_units % step))
    loads[4].wait()
    loads[5].wait()

    @pl.loop(0, width // step)
    def _(n):
        cols = pl.ds(pl.multiple_of(n * step, step), step)
        expert = jnp.dot(hid[...], ed[:, cols], preferred_element_type=jnp.float32)
        dense = jnp.dot(dhid[...], dd[:, cols], preferred_element_type=jnp.float32)
        both = wcol[:, :1] * expert + jax.nn.sigmoid(mix_ref[:, cols]) * dense
        both = both.reshape(E, T, rows, step).astype(jnp.bfloat16)
        for j in range(T):
            cbuf[j % 2, j // 2, :, :, cols] = both[:, j]

    others = []
    for k in range(Y):
        yy = (y + 1 + k) % Y
        cp = rcopy(cbuf.at[1 - c, yy], crecv.at[yy], cr_s.at[yy], cr_r.at[yy], e, partner)
        cp.start()
        sends.append(cp)
        others.append(yy)

    def core_sum(yy, block):
        return cbuf[c, yy, block].astype(jnp.float32) + crecv[yy, block].astype(jnp.float32)

    def core_arrived(yy):
        rcopy(crecv.at[yy], crecv.at[yy], cr_s.at[yy], cr_r.at[yy], e, partner).wait_recv()

    for yy in others[:-1]:
        core_arrived(yy)
        for i in far + [0]:
            block = (e + i) % E
            ysend[yy, block] = core_sum(yy, block).astype(jnp.bfloat16)
            cp = rcopy(
                ysend.at[yy, block], yrecv.at[y, block], yr_s.at[yy, block], yr_r.at[y, block], e, yy * 2 + c
            )
            cp.start()
            sends.append(cp)
    core_arrived(y)
    total = None
    for i in far + [0]:
        block = (e + i) % E
        total = core_sum(y, block)
        for yy in others[:-1]:
            rcopy(
                yrecv.at[yy, block], yrecv.at[yy, block], yr_s.at[yy, block], yr_r.at[yy, block], e, yy * 2 + c
            ).wait_recv()
            total = total + yrecv[yy, block].astype(jnp.float32)
        if i:
            esend[block] = total.astype(jnp.bfloat16)
            cp = rcopy(esend.at[block], erecv.at[e], er_s.at[block], er_r.at[e], block, t)
            cp.start()
            sends.append(cp)
    total = total + resid_ref[...]
    for i in near:
        source = (e + i) % E
        rcopy(erecv.at[source], erecv.at[source], er_s.at[source], er_r.at[source], source, t).wait_recv()
        total = total + erecv[source].astype(jnp.float32)
    fbuf[t] = total.astype(jnp.bfloat16)
    for i in range(1, T):
        j = (t + i) % T
        cp = rcopy(fbuf.at[t], fbuf.at[t], f_s.at[j], f_r.at[t], e, j)
        cp.start()
        sends.append(cp)
    for i in range(1, T):
        j = (t + i) % T
        rcopy(fbuf.at[j], fbuf.at[j], f_s.at[j], f_r.at[j], e, j).wait_recv()
    out_ref[...] = fbuf[...]
    for cp in sends:
        cp.wait_send()


def channel_mixers(tokens, term, ffn_gain, dense_mix, routes, route_weights, expert, dense):
    E, T = lax.axis_size("ep"), lax.axis_size("tp")
    Y = T // 2
    seqs, width = tokens.shape
    rows = seqs // T
    eg, eu, ed = expert
    dg, du, dd = dense
    units = dg.shape[0] // T
    hidden_units = eg.shape[1]
    bf, f32 = jnp.bfloat16, jnp.float32
    vmem, dma = pltpu.VMEM, pltpu.SemaphoreType.DMA
    block = (rows, width)
    total = E * seqs
    vm = pl.BlockSpec(memory_space=pltpu.VMEM)
    hbm = pl.BlockSpec(memory_space=pl.ANY)
    out = pl.pallas_call(
        functools.partial(channel_kernel, E, T),
        out_shape=jax.ShapeDtypeStruct((T,) + block, bf),
        in_specs=[vm] * 6 + [hbm] * 6,
        out_specs=vm,
        scratch_shapes=[
            vmem(eg.shape, bf),
            vmem(eu.shape, bf),
            vmem(ed.shape, bf),
            vmem((units, width), bf),
            vmem((units, width), bf),
            vmem((units, width), bf),
            vmem((T,) + block, bf),
            vmem((E, T) + block, bf),
            vmem((E, 128), f32),
            vmem((E, E, 128), f32),
            vmem((total, 128), f32),
            vmem((total, width), bf),
            vmem((total, hidden_units), bf),
            vmem((total, units), bf),
            vmem(block, f32),
            vmem((2, Y, E) + block, bf),
            vmem((Y, E) + block, bf),
            vmem((Y, E) + block, bf),
            vmem((Y, E) + block, bf),
            vmem((E,) + block, bf),
            vmem((E,) + block, bf),
            vmem((T,) + block, bf),
            dma((6,)),
            dma((T,)),
            dma((T,)),
            dma((E,)),
            dma((E,)),
            dma((E,)),
            dma((E, T)),
            dma((E, Y)),
            dma((E, Y)),
            dma((Y,)),
            dma((Y,)),
            dma((Y, E)),
            dma((Y, E)),
            dma((E,)),
            dma((E,)),
            dma((T,)),
            dma((T,)),
        ],
        compiler_params=pltpu.CompilerParams(
            collective_id=0, has_side_effects=True, vmem_limit_bytes=62 * 1024 * 1024
        ),
        name="channel_mixers",
    )(
        tokens.reshape((T,) + block),
        term.reshape((T,) + block),
        ffn_gain.reshape(1, width),
        dense_mix.reshape(1, width),
        routes.T,
        route_weights.T,
        eg,
        eu,
        ed,
        dg,
        du,
        dd,
    )
    return out.reshape(seqs, width)


def mixer_kernel(
    chunk,
    tok_ref,
    gain_ref,
    floor_ref,
    hgain_ref,
    wq_hbm,
    wf_hbm,
    wi_hbm,
    wo_hbm,
    w_hbm,
    state_hbm,
    new_hbm,
    term_ref,
    wq,
    wf,
    wi,
    wo,
    w,
    st,
    keep_t,
    query_t,
    vals,
    outgate,
    read_ref,
    w_sem,
    in_sem,
    out_sem,
):
    seqs, heads, key_size, value_size = st.shape
    chunks = seqs // chunk

    def load_state(n):
        at = pl.ds(n * chunk, chunk)
        return pltpu.make_async_copy(state_hbm.at[at], st.at[at], in_sem.at[n])

    def store_state(n):
        at = pl.ds(n * chunk, chunk)
        return pltpu.make_async_copy(st.at[at], new_hbm.at[at], out_sem.at[n])

    load_f = pltpu.make_async_copy(wf_hbm, wf, w_sem.at[0])
    load_q = pltpu.make_async_copy(wq_hbm, wq, w_sem.at[1])
    load_i = pltpu.make_async_copy(wi_hbm, wi, w_sem.at[2])
    load_o = pltpu.make_async_copy(wo_hbm, wo, w_sem.at[3])
    load_w = pltpu.make_async_copy(w_hbm, w, w_sem.at[4])
    load_f.start()
    load_q.start()
    load_i.start()
    for n in range(chunks):
        load_state(n).start()
    load_o.start()
    load_w.start()

    normed = rms_norm(tok_ref[...].astype(jnp.float32), gain_ref[...]).astype(jnp.bfloat16)

    def turned(value, ref):
        for h in range(heads):
            column = value[:, h * key_size : (h + 1) * key_size].T
            for n in range(chunks):
                ref[n, h] = column[:, n * chunk : (n + 1) * chunk]

    load_f.wait()
    zf = jnp.dot(normed, wf[...], preferred_element_type=jnp.float32)
    floor = floor_ref[...]
    turned(floor + (1.0 - floor) * jax.nn.sigmoid(zf), keep_t)
    load_q.wait()
    zq = jnp.dot(normed, wq[...], preferred_element_type=jnp.float32)
    turned(jax.nn.silu(zq), query_t)
    load_i.wait()
    vals[...] = jnp.dot(normed, wi[...], preferred_element_type=jnp.float32)

    @pl.loop(0, chunks)
    def _(n):
        load_state(n).wait()
        first = pl.multiple_of(n * chunk, chunk)
        for h in range(heads):
            lanes = slice(h * value_size, (h + 1) * value_size)
            value = vals[pl.ds(first, chunk), lanes]
            keep = keep_t[n, h]
            query = query_t[n, h]
            reads = []
            for i in range(chunk):
                row = value[i : i + 1]
                new = row + keep[:, i : i + 1] * (st[first + i, h] - row)
                st[first + i, h] = new
                reads.append(jnp.sum(query[:, i : i + 1] * new, axis=0, keepdims=True))
            read_ref[pl.ds(first, chunk), lanes] = jnp.concatenate(reads, axis=0)
        store_state(n).start()

    load_o.wait()
    zg = jnp.dot(normed, wo[...], preferred_element_type=jnp.float32)
    outgate[...] = jax.nn.silu(zg)
    parts = []
    for h in range(heads):
        lanes = slice(h * value_size, (h + 1) * value_size)
        parts.append(rms_norm(read_ref[:, lanes], hgain_ref[...]) * outgate[:, lanes])
    headout = jnp.concatenate(parts, axis=1).astype(jnp.bfloat16)
    load_w.wait()
    term_ref[...] = jnp.dot(headout, w[...], preferred_element_type=jnp.float32).astype(jnp.bfloat16)
    for n in range(chunks):
        store_state(n).wait()


def mixer(tokens, state, norm_gain, weights, forget_floor, head_gain, w_out):
    seqs, width = tokens.shape
    _, heads, key_size, value_size = state.shape
    chunk = 8
    chunks = seqs // chunk
    wq, wf, wi, wo = weights
    f32, bf = jnp.float32, jnp.bfloat16
    vmem, dma = pltpu.VMEM, pltpu.SemaphoreType.DMA
    vm = pl.BlockSpec(memory_space=pltpu.VMEM)
    hbm = pl.BlockSpec(memory_space=pl.ANY)
    return pl.pallas_call(
        functools.partial(mixer_kernel, chunk),
        out_shape=(
            jax.ShapeDtypeStruct(state.shape, f32),
            jax.ShapeDtypeStruct((seqs, width), bf),
        ),
        in_specs=[vm] * 4 + [hbm] * 6,
        out_specs=(hbm, vm),
        scratch_shapes=[
            vmem(wq.shape, bf),
            vmem(wf.shape, bf),
            vmem(wi.shape, bf),
            vmem(wo.shape, bf),
            vmem(w_out.shape, bf),
            vmem(state.shape, f32),
            vmem((chunks, heads, key_size, chunk), f32),
            vmem((chunks, heads, key_size, chunk), f32),
            vmem((seqs, heads * value_size), f32),
            vmem((seqs, heads * value_size), f32),
            vmem((seqs, heads * value_size), f32),
            dma((5,)),
            dma((chunks,)),
            dma((chunks,)),
        ],
        compiler_params=pltpu.CompilerParams(vmem_limit_bytes=60 * 1024 * 1024),
        name="mixer",
    )(
        tokens,
        norm_gain.reshape(1, width),
        forget_floor.reshape(1, heads * key_size),
        head_gain.reshape(1, value_size),
        wq,
        wf,
        wi,
        wo,
        w_out,
        state,
    )


def local(
    tokens,
    state,
    norm_gain,
    w_query,
    w_forget,
    w_input,
    w_outgate,
    forget_floor,
    head_gain,
    w_out,
    ffn_gain,
    routes,
    route_weights,
    expert_gate,
    expert_up,
    expert_down,
    dense_gate,
    dense_up,
    dense_down,
    dense_mix,
):
    seqs, width = tokens.shape
    resid_in = tokens.astype(jnp.float32)
    new_state, block_term = mixer(
        tokens,
        state,
        norm_gain,
        (w_query, w_forget, w_input, w_outgate),
        forget_floor,
        head_gain,
        w_out,
    )
    ways = lax.axis_size("tp")
    if ways % 2 == 0 and seqs % (8 * ways) == 0 and dense_gate.shape[1] % (16 * ways) == 0:
        mixed = channel_mixers(
            tokens,
            block_term,
            ffn_gain,
            dense_mix,
            routes,
            route_weights,
            (expert_gate[0], expert_up[0], expert_down[0]),
            (dense_gate.T, dense_up.T, dense_down),
        )
        return (mixed, new_state)
    mixout = lax.psum(block_term, "tp").astype(jnp.float32)
    resid = resid_in + mixout
    ffn_in = rms_norm(resid, ffn_gain).astype(jnp.bfloat16)
    piece = lax.all_gather(ffn_in, "ep", axis=0, tiled=True)
    dgate = jnp.dot(piece, dense_gate, preferred_element_type=jnp.float32)
    dupper = jnp.dot(piece, dense_up, preferred_element_type=jnp.float32)
    dense_hidden = (jax.nn.silu(dgate) * dupper).astype(jnp.bfloat16)
    rows = dense_hidden
    summed = lax.psum_scatter(
        jnp.dot(rows, dense_down, preferred_element_type=jnp.float32).astype(jnp.bfloat16),
        "ep",
        scatter_dimension=0,
        tiled=True,
    )
    dense = summed.astype(jnp.float32)
    experts = lax.axis_size("ep") * expert_gate.shape[0]
    top = routes.shape[1]
    capacity = 2 * seqs * top // experts
    table = make_table(routes, experts, capacity)
    repeated = jnp.repeat(ffn_in, top, axis=0)
    sent = jnp.dot(table.T, repeated, preferred_element_type=jnp.float32).astype(jnp.bfloat16)
    sent = sent.reshape(experts, capacity, width)
    arrived = lax.all_to_all(sent, "ep", split_axis=0, concat_axis=0, tiled=True)
    sources, items, _ = arrived.shape
    rows = arrived.reshape(sources * items, width)
    gate = jnp.dot(rows, expert_gate[0], preferred_element_type=jnp.float32)
    upper = jnp.dot(rows, expert_up[0], preferred_element_type=jnp.float32)
    hidden = (jax.nn.silu(gate) * upper).astype(jnp.bfloat16)
    part = jnp.dot(hidden, expert_down[0], preferred_element_type=jnp.float32)
    part = part.astype(jnp.bfloat16).astype(jnp.float32)
    summed_parts = lax.psum(part.astype(jnp.bfloat16), "tp")
    results = summed_parts.reshape(sources, items, width)
    back = lax.all_to_all(results, "ep", split_axis=0, concat_axis=0, tiled=True)
    picked = jnp.dot(
        table, back.reshape(experts * capacity, width), preferred_element_type=jnp.float32
    )
    weighted = picked * route_weights.reshape(seqs * top)[:, None]
    moe = jnp.sum(weighted.reshape(seqs, top, width), axis=1)
    mixed = (resid + moe + jax.nn.sigmoid(dense_mix) * dense).astype(jnp.bfloat16)
    return (mixed, new_state)


def solution(mesh):
    in_specs = (
        P("ep", None),
        P("ep", "tp", None, None),
        P(),
        P(None, "tp"),
        P(None, "tp"),
        P(None, "tp"),
        P(None, "tp"),
        P("tp"),
        P(),
        P("tp", None),
        P(),
        P("ep", None),
        P("ep", None),
        P("ep", None, "tp"),
        P("ep", None, "tp"),
        P("ep", "tp", None),
        P(None, "ep"),
        P(None, "ep"),
        P("ep", None),
        P(),
    )
    out_specs = (P("ep", None), P("ep", "tp", None, None))
    return jax.shard_map(local, mesh=mesh, in_specs=in_specs, out_specs=out_specs, check_vma=False)
```
